32 devices in a mesh: ep: 8 (over z, x), tp: 4 (over y, core).
Axes of the slice: x: 2, y: 2, z: 4, core: 2. Of those that a mesh axis runs over, the one named last changes fastest.
Arguments:
- tokens: bfloat16 [4608, 2048], P(('ep', 'tp')), may hold values from -6 to 6
- norm_gain: float32 [2048], replicated, may hold values from 0.1 to 1.9
- expert_ids: int32 [4608, 8], P(('ep', 'tp')), may hold values from 0 to 15, all different within a row; in each aligned block of 144 rows (0 to 143, 144 to 287, ...) at most 144 rows name the same one
- route_weights: float32 [4608, 8], P(('ep', 'tp')), may hold values from 0.3 to 1
- expert_gate: bfloat16 [16, 512, 2048], P('ep', 'tp'), may hold values from -0.125 to 0.125
- expert_up: bfloat16 [16, 512, 2048], P('ep', 'tp'), may hold values from -0.125 to 0.125
- expert_down: bfloat16 [16, 512, 2048], P('ep', 'tp'), may hold values from -0.25 to 0.25
- shared_gate: bfloat16 [512, 2048], P('tp'), may hold values from -0.125 to 0.125
- shared_up: bfloat16 [512, 2048], P('tp'), may hold values from -0.125 to 0.125
- shared_down: bfloat16 [512, 2048], P('tp'), may hold values from -0.25 to 0.25
- side_in: bfloat16 [2048, 1024], P('ep'), may hold values from -0.125 to 0.125
- side_out: bfloat16 [2048, 1024], P('ep'), may hold values from -0.1875 to 0.1875
- side_gate: bfloat16 [2048], replicated, may hold values from -0.125 to 0.125
Outputs:
- mixed: bfloat16 [4608, 2048], P(('ep', 'tp'))
The draws below stay inside these ranges and needn't reach their ends.
Inputs may be any that keep to these rules, and one draw needn't show every extreme that they name: `expert_ids`: each row names 8 different experts of 0 to 15; within the rows of one device (aligned blocks of 144 rows) no expert is named more than 144 times, and in some of those blocks some expert is named exactly 144 times.
All inputs are finite; a program needn't handle non-finite values.
Results may differ from the reference program's by a relative error of at most 0.0068.
Values may be sent and summed in bfloat16 or wider, within the bound.
No kernel may reach another device: no remote copies, remote signals or barrier semaphores. Data moves between devices by JAX's collectives and lax.ppermute only.
A program may use at most 320 MiB of HBM per device.

```python
import math
import jax
import jax.numpy as jnp
import numpy as np
from jax import lax

D = 2048
FF = 512
SIDE = 1024
TOP = 8
TOK_DEV = 144
EXPERTS = 16
CAP = 144
TOKENS = 4608


def levels(stream_key, extent, pieces, smallest, largest):
    level = 1.0
    for dim, blocks in pieces:
        steps = jax.random.uniform(jax.random.fold_in(jax.random.fold_in(stream_key, 6), dim), (blocks,), jnp.float32, smallest / len(pieces), largest / len(pieces))
        level = level * jnp.repeat(jnp.exp(steps), extent[dim] // blocks).reshape((-1,) + (1,) * (len(extent) - 1 - dim))
    return level


def shared_out(rng, own, number, rows, number_of, top, bound, skew):
    ranking = jax.random.permutation(rng, number_of)
    heavy_load, common = portions_of(number_of, rows * top, bound, skew, True), portions_of(number_of, rows * top, bound, skew, False)
    places = jnp.arange(number_of)

    def named(lengths, rotation):
        used = int((lengths > 0).sum())
        fixed = max(1, used // 4)
        shifted = fixed + (places - fixed + rotation * (used - fixed)) % max(1, number_of - fixed)
        return jnp.zeros((number_of,), jnp.int32).at[ranking[jnp.where(places < fixed, places, shifted)]].set(jnp.asarray(lengths, jnp.int32))

    lengths = jnp.where(number % 4 == 0, named(heavy_load, number // 4), named(common, number - number // 4 - 1))
    mixed = jax.random.permutation(jax.random.fold_in(own, 3), number_of)
    source_of, receiver = mixed[0:number_of // 2 * 2:2], mixed[1:number_of // 2 * 2:2]
    slack = jnp.minimum(lengths[source_of] - 1, bound - lengths[receiver]) // 2
    slack = jnp.where((source_of == ranking[0]) | (receiver == ranking[0]) | (lengths[receiver] == 0), 0, jnp.maximum(slack, 0))
    shifted = jax.random.randint(jax.random.fold_in(own, 4), (number_of // 2,), 0, 1 << 20) % (slack + 1)
    lengths = lengths.at[source_of].add(-shifted).at[receiver].add(shifted)
    items = jnp.searchsorted(jnp.cumsum(lengths), jnp.arange(rows * top), side="right").astype(jnp.int32)
    listing = items.reshape(top, rows).T
    listing = listing[jax.random.permutation(jax.random.fold_in(own, 1), rows)]
    rotation = jax.random.randint(jax.random.fold_in(own, 2), (rows, 1), 0, top)
    return jnp.take_along_axis(listing, (jnp.arange(top)[None, :] + rotation) % top, axis=1)


def portions_of(amount, total, reach, slope, full):
    loads = [(1 << 20) // math.isqrt(rank ** slope) + 1 for rank in range(1, amount + 1)]
    largest = reach if full else min(reach, max(-(-total // amount), total * loads[0] // sum(loads)))
    least = 1 if total - largest >= amount - 1 else 0
    holding, spare = [largest] + [least] * (amount - 1), total - largest - least * (amount - 1)
    while spare > 0:
        free = [i for i in range(1, amount) if holding[i] < largest] or [i for i in range(1, amount) if holding[i] < reach]
        pool, left = sum([loads[i] for i in free]), spare
        for i in free:
            addition = min(reach - holding[i], max(1, left * loads[i] // pool), spare)
            holding[i] = holding[i] + addition
            spare = spare - addition
    return np.array(holding)


def centred(key, dims, scale, reach, split=(), kind=jnp.bfloat16):
    gain = levels(key, dims, split, -0.22, 0.18) if split else 1.0
    array = jax.random.normal(key, dims, jnp.float32) * scale * gain
    return jnp.minimum(jnp.maximum(array, -reach), reach).astype(kind)


def setup_inputs(seed: int = 0) -> dict:
    arg_keys = jax.random.split(jax.random.key(seed), 14)
    tokens = centred(arg_keys[0], (TOKENS, D), 1.0, 6.0, ((0, 32),))
    norm_gain = jnp.clip(1.0 + 0.18 * jax.random.normal(arg_keys[1], (D,), jnp.float32), 0.1, 1.9)
    expert_ids_keys = jax.random.split(jax.random.fold_in(arg_keys[2], 1), TOKENS // TOK_DEV)
    expert_ids_turns = jax.random.permutation(jax.random.fold_in(arg_keys[2], 3), TOKENS // TOK_DEV)
    expert_ids = jax.vmap(lambda own, number: shared_out(jax.random.fold_in(arg_keys[2], 2), own, number, TOK_DEV, EXPERTS, TOP, CAP, 2))(expert_ids_keys, expert_ids_turns).reshape((TOKENS, TOP))
    route_weights = jnp.clip(0.3 + 0.7 * jax.random.uniform(arg_keys[3], (TOKENS, TOP), jnp.float32) ** levels(arg_keys[3], (TOKENS, TOP), ((0, 32),), -0.2, 0.2), 0.3, 1.0)
    expert_gate = centred(arg_keys[4], (EXPERTS, FF, D), D ** -0.5, 0.125, ((0, 8), (1, 4)))
    expert_up = centred(arg_keys[5], (EXPERTS, FF, D), D ** -0.5, 0.125, ((0, 8), (1, 4)))
    expert_down = centred(arg_keys[6], (EXPERTS, FF, D), FF ** -0.5, 0.25, ((0, 8), (1, 4)))
    shared_gate = centred(arg_keys[7], (FF, D), D ** -0.5, 0.125, ((0, 4),))
    shared_up = centred(arg_keys[8], (FF, D), D ** -0.5, 0.125, ((0, 4),))
    shared_down = centred(arg_keys[9], (FF, D), FF ** -0.5, 0.25, ((0, 4),))
    side_in = centred(arg_keys[10], (D, SIDE), D ** -0.5, 0.125, ((0, 8),))
    side_out = centred(arg_keys[11], (D, SIDE), SIDE ** -0.5, 0.1875, ((0, 8),))
    side_gate = centred(arg_keys[12], (D,), D ** -0.5, 0.125)
    return dict(tokens=tokens, norm_gain=norm_gain, expert_ids=expert_ids, route_weights=route_weights, expert_gate=expert_gate, expert_up=expert_up, expert_down=expert_down, shared_gate=shared_gate, shared_up=shared_up, shared_down=shared_down, side_in=side_in, side_out=side_out, side_gate=side_gate)


norm_eps = 1.0
row_block = 512

def normalize(tokens, norm_gain):
    values = tokens.astype(jnp.float32)
    scale_inv = lax.rsqrt(lax.optimization_barrier(jnp.mean(values * values, axis=-1, keepdims=True)) + norm_eps)
    return (values * scale_inv * norm_gain).astype(jnp.bfloat16)

def swiglu(gate_part, up_part):
    return (jax.nn.silu(gate_part) * up_part).astype(jnp.bfloat16)

def reference(tokens, norm_gain, expert_ids, route_weights, expert_gate, expert_up, expert_down, shared_gate, shared_up, shared_down, side_in, side_out, side_gate):
    normed = normalize(tokens, norm_gain)
    pair_count = TOKENS * TOP
    flat_ids = expert_ids.reshape(pair_count).astype(jnp.int32)
    flat_tokens = (jnp.arange(pair_count, dtype=jnp.int32) // TOP).astype(jnp.int32)
    flat_weights = route_weights.reshape(pair_count)
    order = jnp.argsort(flat_ids, stable=True)
    sorted_ids = flat_ids[order]
    counts = jnp.bincount(flat_ids, length=EXPERTS).astype(jnp.int32)
    starts = (jnp.cumsum(counts) - counts).astype(jnp.int32)
    padded = ((counts + row_block - 1) // row_block * row_block).astype(jnp.int32)
    ends = jnp.cumsum(padded).astype(jnp.int32)
    begins = (ends - padded).astype(jnp.int32)
    target = (begins[sorted_ids] + jnp.arange(pair_count, dtype=jnp.int32) - starts[sorted_ids]).astype(jnp.int32)
    block_count = (pair_count + EXPERTS * (row_block - 1)) // row_block + 1
    slots_all = block_count * row_block
    token_slots = jnp.full((slots_all,), TOKENS, jnp.int32).at[target].set(flat_tokens[order])
    weight_slots = jnp.zeros((slots_all,), jnp.float32).at[target].set(flat_weights[order])
    block_starts = (jnp.arange(block_count, dtype=jnp.int32) * row_block).astype(jnp.int32)
    block_expert = jnp.minimum(jnp.searchsorted(ends, block_starts, side='right'), EXPERTS - 1).astype(jnp.int32)
    extended = jnp.concatenate([normed, jnp.zeros((1, D), normed.dtype)], axis=0)

    def block_step(running, inputs):
        slot_tokens, slot_weights, expert = inputs
        chosen = extended[slot_tokens]
        gate_part = jnp.dot(chosen, expert_gate[expert].T, preferred_element_type=jnp.float32)
        up_part = jnp.dot(chosen, expert_up[expert].T, preferred_element_type=jnp.float32)
        hidden = swiglu(gate_part, up_part)
        output = jnp.dot(hidden, expert_down[expert], preferred_element_type=jnp.float32).astype(jnp.bfloat16)
        output = lax.optimization_barrier(output).astype(jnp.float32)
        return (running.at[slot_tokens].add(output * slot_weights[:, None]), None)
    running = jnp.zeros((TOKENS + 1, D), jnp.float32)
    running, unused = lax.scan(block_step, running, (token_slots.reshape(block_count, row_block), weight_slots.reshape(block_count, row_block), block_expert))
    routed = running[:TOKENS]
    shared_hidden = swiglu(jnp.dot(normed, shared_gate.T, preferred_element_type=jnp.float32), jnp.dot(normed, shared_up.T, preferred_element_type=jnp.float32))
    shared = jnp.dot(shared_hidden, shared_down, preferred_element_type=jnp.float32)
    side_hidden = jax.nn.silu(jnp.dot(normed, side_in, preferred_element_type=jnp.float32)).astype(jnp.bfloat16)
    side_value = jnp.dot(side_hidden, side_out.T, preferred_element_type=jnp.float32)
    opening = jax.nn.sigmoid(jnp.dot(normed, side_gate, preferred_element_type=jnp.float32))
    return (routed + shared + opening[:, None] * side_value).astype(jnp.bfloat16)
```

```python
import jax
import jax.numpy as jnp
from jax import lax
from jax.sharding import PartitionSpec as P

norm_eps = 1.0
cores = 2


def normalize(tokens, norm_gain):
    values = tokens.astype(jnp.float32)
    scale_inv = lax.rsqrt(jnp.mean(values * values, axis=-1, keepdims=True) + norm_eps)
    return (values * scale_inv * norm_gain).astype(jnp.bfloat16)


def over_y(piece):
    size = lax.axis_size("tp")
    places = size // cores
    return [
        lax.ppermute(
            piece,
            "tp",
            [(s, (s // cores + r) % places * cores + s % cores) for s in range(size)],
        )
        for r in range(1, places)
    ]


def over_core(piece):
    size = lax.axis_size("tp")
    return lax.ppermute(piece, "tp", [(s, s // cores * cores + (s + 1) % cores) for s in range(size)])


def rows_dot(left, right):
    return lax.dot_general(
        left, right, (((1,), (1,)), ((), ())), preferred_element_type=jnp.float32
    )


def body(
    tokens,
    norm_gain,
    expert_ids,
    route_weights,
    expert_gate,
    expert_up,
    expert_down,
    shared_gate,
    shared_up,
    shared_down,
    side_in,
    side_out,
    side_gate,
):
    groups = lax.axis_size("ep")
    rank = lax.axis_index("ep")
    local_experts, hidden_part, width = expert_gate.shape
    experts_all = groups * local_experts

    normed = normalize(tokens, norm_gain)
    every = lax.all_gather(normed, "ep", axis=0, tiled=True)

    chosen = expert_ids[:, :, None] == jnp.arange(experts_all, dtype=jnp.int32)[None, None, :]
    dense = jnp.sum(jnp.where(chosen, route_weights[:, :, None], 0.0), axis=1)
    opening = jax.nn.sigmoid(jnp.dot(normed, side_gate, preferred_element_type=jnp.float32))
    factors = lax.all_gather(
        jnp.concatenate([dense, opening[:, None]], axis=1), "ep", axis=0, tiled=True
    )
    mine = lax.dynamic_slice_in_dim(factors, rank * local_experts, local_experts, axis=1)
    opened = factors[:, experts_all:]

    flat = [w.reshape(local_experts * hidden_part, width) for w in (expert_gate, expert_up, expert_down)]
    far = [over_y(w) for w in flat]
    near = [[w, over_core(w)] for w in flat]
    far = [[q for p in w for q in (p, over_core(p))] for w in far]

    unit_count = shared_gate.shape[0] // groups
    shared_units = jnp.stack(
        [
            lax.dynamic_slice_in_dim(w, rank * unit_count, unit_count, axis=0)
            for w in (shared_gate, shared_up, shared_down)
        ]
    )
    shared_units = lax.all_gather(shared_units, "tp", axis=1, tiled=True)

    side_units = side_in.shape[1] // groups
    both = jnp.stack([side_in, side_out]).reshape(2, side_in.shape[0], groups, side_units)
    both = lax.all_to_all(both, "ep", split_axis=2, concat_axis=1, tiled=True)
    both = both.reshape(2, width, side_units)

    def routed_hidden(gate, up):
        gate_part, up_part = rows_dot(every, gate), rows_dot(every, up)
        place = lax.broadcasted_iota(jnp.int32, (1, gate.shape[0]), 1) // hidden_part % local_experts
        scale = mine[:, 0:1]
        for e in range(1, local_experts):
            scale = jnp.where(place == e, mine[:, e : e + 1], scale)
        return (jax.nn.silu(gate_part) * up_part * scale).astype(jnp.bfloat16)

    near_gate, near_up, near_down = [jnp.concatenate(w) for w in near]
    far_gate, far_up, far_down = [jnp.concatenate(w) for w in far]

    hidden = routed_hidden(near_gate, near_up)
    total = jnp.dot(hidden, near_down, preferred_element_type=jnp.float32)
    shared_hidden = (
        jax.nn.silu(rows_dot(every, shared_units[0])) * rows_dot(every, shared_units[1])
    ).astype(jnp.bfloat16)
    total += jnp.dot(shared_hidden, shared_units[2], preferred_element_type=jnp.float32)
    side_hidden = (
        jax.nn.silu(jnp.dot(every, both[0], preferred_element_type=jnp.float32)) * opened
    ).astype(jnp.bfloat16)
    total += rows_dot(side_hidden, both[1])
    hidden = routed_hidden(far_gate, far_up)
    total += jnp.dot(hidden, far_down, preferred_element_type=jnp.float32)
    return lax.psum_scatter(total.astype(jnp.bfloat16), "ep", scatter_dimension=0, tiled=True)


def solution(mesh):
    placed = (
        P(("ep", "tp"), None),
        P(),
        P(("ep", "tp"), None),
        P(("ep", "tp"), None),
        P("ep", "tp", None),
        P("ep", "tp", None),
        P("ep", "tp", None),
        P("tp", None),
        P("tp", None),
        P("tp", None),
        P("ep", None),
        P("ep", None),
        P(),
    )
    return jax.shard_map(
        body, mesh=mesh, in_specs=placed, out_specs=P(("ep", "tp"), None), check_vma=False
    )
```

```python
import jax
import jax.numpy as jnp
from jax import lax
from jax.experimental import pallas as pl
from jax.experimental.pallas import tpu as pltpu
from jax.sharding import PartitionSpec as P

norm_eps = 1.0
cores = 2
lanes = 128
per_call = 2


def normalize(tokens, norm_gain):
    values = tokens.astype(jnp.float32)
    scale_inv = lax.rsqrt(jnp.mean(values * values, axis=-1, keepdims=True) + norm_eps)
    return (values * scale_inv * norm_gain).astype(jnp.bfloat16)


def rotate(piece, axis, outer, inner, by_outer, by_inner):
    pairs = [
        (s, (s // inner + by_outer) % outer * inner + (s % inner + by_inner) % inner)
        for s in range(outer * inner)
    ]
    return lax.ppermute(piece, axis, pairs)


def rows_dot(left, right):
    return lax.dot_general(
        left, right, (((1,), (1,)), ((), ())), preferred_element_type=jnp.float32
    )


def experts(rows, gates, ups, downs, shared_up_gate, shared_down, side_in, side_out, select):
    count, pieces = len(rows), len(gates)
    block, wide = rows[0].shape
    units, width = gates[0].shape
    shared_units, side_units = shared_down.shape[0], side_in.shape[1]
    everything = count * block
    chunk = 512 if width % 512 == 0 else width

    def kernel(*refs):
        refs = list(refs)
        take = lambda n: [refs.pop(0) for _ in range(n)]
        row_refs, gate_refs, up_refs, down_refs = take(count), take(pieces), take(pieces), take(pieces)
        both_ref, shared_ref, in_ref, out_ref, select_ref = take(5)
        outs = take(count)
        x, gate, up, down, hidden, hidden_shared, hidden_side, sems = refs
        row_copies = [
            pltpu.make_async_copy(row_refs[i], x.at[pl.ds(i * block, block)], sems.at[0, i])
            for i in range(count)
        ]
        copies = [
            [pltpu.make_async_copy(src[p], dst.at[p], sems.at[k + 1, p]) for p in range(pieces)]
            for k, (src, dst) in enumerate(((gate_refs, gate), (up_refs, up), (down_refs, down)))
        ]
        for c in row_copies:
            c.start()
        for p in range(pieces):
            copies[0][p].start()
            copies[1][p].start()
        for p in range(pieces):
            copies[2][p].start()
        for c in row_copies:
            c.wait()

        def scale_of(start, size):
            return jnp.dot(
                x[:, width:], select_ref[:, start : start + size], preferred_element_type=jnp.float32
            )

        start = pieces * units
        pair = rows_dot(x[:, :width], both_ref[...])
        gate_part, up_part = pair[:, :shared_units], pair[:, shared_units:]
        hidden_shared[...] = (jax.nn.silu(gate_part) * up_part).astype(jnp.bfloat16)
        side = jnp.dot(x[:, :width], in_ref[...], preferred_element_type=jnp.float32)
        hidden_side[...] = (jax.nn.silu(side) * scale_of(start, side_units)).astype(jnp.bfloat16)
        for p in range(pieces):
            copies[0][p].wait()
            copies[1][p].wait()
            gate_part = rows_dot(x[:, :width], gate[p])
            up_part = rows_dot(x[:, :width], up[p])
            scale = scale_of(p * units, units)
            hidden[p] = (jax.nn.silu(gate_part) * up_part * scale).astype(jnp.bfloat16)
        for p in range(pieces):
            copies[2][p].wait()
        for n in range(0, width, chunk):
            total = rows_dot(hidden_side[...], out_ref[n : n + chunk, :])
            total += jnp.dot(
                hidden_shared[...], shared_ref[:, n : n + chunk], preferred_element_type=jnp.float32
            )
            for p in range(pieces):
                total += jnp.dot(
                    hidden[p], down[p, :, n : n + chunk], preferred_element_type=jnp.float32
                )
            for i in range(count):
                outs[i][:, n : n + chunk] = total[i * block : (i + 1) * block].astype(jnp.bfloat16)

    anywhere = pl.BlockSpec(memory_space=pl.ANY)
    inside = pl.BlockSpec(memory_space=pltpu.VMEM)
    flops = 2 * everything * width * (3 * (pieces * units + shared_units) + 2 * side_units)
    return pl.pallas_call(
        kernel,
        out_shape=[jax.ShapeDtypeStruct((block, width), jnp.bfloat16)] * count,
        in_specs=[anywhere] * (count + 3 * pieces) + [inside] * 5,
        out_specs=[inside] * count,
        scratch_shapes=[
            pltpu.VMEM((everything, wide), jnp.bfloat16),
            pltpu.VMEM((pieces, units, width), jnp.bfloat16),
            pltpu.VMEM((pieces, units, width), jnp.bfloat16),
            pltpu.VMEM((pieces, units, width), jnp.bfloat16),
            pltpu.VMEM((pieces, everything, units), jnp.bfloat16),
            pltpu.VMEM((everything, shared_units), jnp.bfloat16),
            pltpu.VMEM((everything, side_units), jnp.bfloat16),
            pltpu.SemaphoreType.DMA((4, max(count, pieces))),
        ],
        compiler_params=pltpu.CompilerParams(vmem_limit_bytes=56 * 1024 * 1024),
        cost_estimate=pl.CostEstimate(
            flops=flops, transcendentals=0, bytes_accessed=6 * pieces * units * width
        ),
    )(*rows, *gates, *ups, *downs, shared_up_gate, shared_down, side_in, side_out, select)


def body(
    tokens,
    norm_gain,
    expert_ids,
    route_weights,
    expert_gate,
    expert_up,
    expert_down,
    shared_gate,
    shared_up,
    shared_down,
    side_in,
    side_out,
    side_gate,
):
    groups, members = lax.axis_size("ep"), lax.axis_size("tp")
    rank = lax.axis_index("ep")
    local_experts, hidden_part, width = expert_gate.shape
    experts_all = groups * local_experts
    zs = 1
    while zs * zs < groups:
        zs *= 2
    xs, ys = groups // zs, members // cores

    def over_tp(piece):
        same = [piece] + [rotate(piece, "tp", ys, cores, r, 0) for r in range(1, ys)]
        return [q for p in same for q in (p, rotate(p, "tp", ys, cores, 0, 1))]

    normed = normalize(tokens, norm_gain)
    chosen = expert_ids[:, :, None] == jnp.arange(experts_all, dtype=jnp.int32)[None, None, :]
    dense = jnp.sum(jnp.where(chosen, route_weights[:, :, None], 0.0), axis=1)
    opening = jax.nn.sigmoid(jnp.dot(normed, side_gate, preferred_element_type=jnp.float32))
    factors = jnp.concatenate([dense, opening[:, None]], axis=1)
    factor_count = experts_all + 1
    high = lax.reduce_precision(factors, 8, 7)
    low = factors - high
    tail = -(-2 * factor_count // lanes) * lanes
    packed = jnp.pad(jnp.concatenate([high, low], axis=1), ((0, 0), (0, tail - 2 * factor_count)))
    row = jnp.concatenate([normed, packed.astype(jnp.bfloat16)], axis=1)

    along_z = [row] + [rotate(row, "ep", zs, xs, r, 0) for r in range(1, zs)]
    rows = [[r] + [rotate(r, "ep", zs, xs, 0, d) for d in range(1, xs)] for r in along_z]

    flat = [w.reshape(local_experts * hidden_part, width) for w in (expert_gate, expert_up, expert_down)]
    gates, ups, downs = [over_tp(w) for w in flat]

    unit_count = shared_gate.shape[0] // groups
    shared = jnp.stack(
        [
            lax.dynamic_slice_in_dim(w, rank * unit_count, unit_count, axis=0)
            for w in (shared_gate, shared_up, shared_down)
        ]
    )
    shared = jnp.concatenate(over_tp(shared), axis=1)
    both = shared[:2].reshape(2 * unit_count * members, width)

    side_units = side_in.shape[1] // groups
    side = jnp.stack([side_in, side_out]).reshape(2, side_in.shape[0], groups, side_units)
    side = lax.all_to_all(side, "ep", split_axis=2, concat_axis=1, tiled=True)
    side = side.reshape(2, width, side_units)

    units = local_experts * hidden_part
    place = jnp.arange(members * units + side_units, dtype=jnp.int32)
    factor = jnp.where(
        place < members * units, rank * local_experts + place // hidden_part % local_experts, experts_all
    )
    index = jnp.arange(tail, dtype=jnp.int32)[:, None]
    select = ((index == factor) | (index == factor + factor_count)).astype(jnp.bfloat16)

    turns = list(range(1, zs)) + [0]
    collected = {}
    for first in range(0, zs, per_call):
        now = turns[first : first + per_call]
        outs = experts(
            [r for t in now for r in rows[t]], gates, ups, downs, both, shared[2], side[0], side[1], select
        )
        for n, t in enumerate(now):
            blocks = outs[n * xs : (n + 1) * xs]
            total = blocks[0].astype(jnp.float32)
            for d in range(1, xs):
                total += rotate(blocks[d], "ep", zs, xs, 0, -d).astype(jnp.float32)
            if t:
                collected[t] = rotate(total.astype(jnp.bfloat16), "ep", zs, xs, -t, 0)
            else:
                collected[t] = total
    mixed = collected[0]
    for t in range(1, zs):
        mixed += collected[t].astype(jnp.float32)
    return mixed.astype(jnp.bfloat16)


def solution(mesh):
    placed = (
        P(("ep", "tp"), None),
        P(),
        P(("ep", "tp"), None),
        P(("ep", "tp"), None),
        P("ep", "tp", None),
        P("ep", "tp", None),
        P("ep", "tp", None),
        P("tp", None),
        P("tp", None),
        P("tp", None),
        P("ep", None),
        P("ep", None),
        P(),
    )
    return jax.shard_map(
        body, mesh=mesh, in_specs=placed, out_specs=P(("ep", "tp"), None), check_vma=False
    )
```

```python
import jax
import jax.numpy as jnp
from jax import lax
from jax.experimental import pallas as pl
from jax.experimental.pallas import tpu as pltpu
from jax.sharding import PartitionSpec as P

norm_eps = 1.0
cores = 2
lanes = 128


def normalize(tokens, norm_gain):
    values = tokens.astype(jnp.float32)
    scale_inv = lax.rsqrt(jnp.mean(values * values, axis=-1, keepdims=True) + norm_eps)
    return (values * scale_inv * norm_gain).astype(jnp.bfloat16)


def rotate(piece, axis, outer, inner, by_outer, by_inner):
    pairs = [
        (s, (s // inner + by_outer) % outer * inner + (s % inner + by_inner) % inner)
        for s in range(outer * inner)
    ]
    return lax.ppermute(piece, axis, pairs)


def rows_dot(left, right):
    return lax.dot_general(
        left, right, (((1,), (1,)), ((), ())), preferred_element_type=jnp.float32
    )


def experts(rows, gates, ups, downs, shared_up_gate, shared_down, side_in, side_out, select):
    count, pieces = len(rows), len(gates)
    block, wide = rows[0].shape
    units, width = gates[0].shape
    shared_units, side_units = shared_down.shape[0], side_in.shape[1]
    everything = count * block
    chunk = 512 if width % 512 == 0 else width

    def kernel(*refs):
        refs = list(refs)
        take = lambda n: [refs.pop(0) for _ in range(n)]
        row_refs, gate_refs, up_refs, down_refs = take(count), take(pieces), take(pieces), take(pieces)
        both_ref, shared_ref, in_ref, out_ref, select_ref = take(5)
        outs = take(count)
        x, gate, up, down, hidden, hidden_shared, hidden_side, sems = refs
        row_copies = [
            pltpu.make_async_copy(row_refs[i], x.at[pl.ds(i * block, block)], sems.at[0, i])
            for i in range(count)
        ]
        copies = [
            [pltpu.make_async_copy(src[p], dst.at[p], sems.at[k + 1, p]) for p in range(pieces)]
            for k, (src, dst) in enumerate(((gate_refs, gate), (up_refs, up), (down_refs, down)))
        ]
        for c in row_copies:
            c.start()
        for p in range(pieces):
            copies[0][p].start()
            copies[1][p].start()
        for p in range(pieces):
            copies[2][p].start()
        for c in row_copies:
            c.wait()

        def scale_of(start, size):
            return jnp.dot(
                x[:, width:], select_ref[:, start : start + size], preferred_element_type=jnp.float32
            )

        start = pieces * units
        pair = rows_dot(x[:, :width], both_ref[...])
        gate_part, up_part = pair[:, :shared_units], pair[:, shared_units:]
        hidden_shared[...] = (jax.nn.silu(gate_part) * up_part).astype(jnp.bfloat16)
        side = jnp.dot(x[:, :width], in_ref[...], preferred_element_type=jnp.float32)
        hidden_side[...] = (jax.nn.silu(side) * scale_of(start, side_units)).astype(jnp.bfloat16)
        for p in range(pieces):
            copies[0][p].wait()
            copies[1][p].wait()
            gate_part = rows_dot(x[:, :width], gate[p])
            up_part = rows_dot(x[:, :width], up[p])
            scale = scale_of(p * units, units)
            hidden[p] = (jax.nn.silu(gate_part) * up_part * scale).astype(jnp.bfloat16)
        for p in range(pieces):
            copies[2][p].wait()
        for n in range(0, width, chunk):
            total = rows_dot(hidden_side[...], out_ref[n : n + chunk, :])
            total += jnp.dot(
                hidden_shared[...], shared_ref[:, n : n + chunk], preferred_element_type=jnp.float32
            )
            for p in range(pieces):
                total += jnp.dot(
                    hidden[p], down[p, :, n : n + chunk], preferred_element_type=jnp.float32
                )
            for i in range(count):
                outs[i][:, n : n + chunk] = total[i * block : (i + 1) * block].astype(jnp.bfloat16)

    anywhere = pl.BlockSpec(memory_space=pl.ANY)
    inside = pl.BlockSpec(memory_space=pltpu.VMEM)
    flops = 2 * everything * width * (3 * (pieces * units + shared_units) + 2 * side_units)
    return pl.pallas_call(
        kernel,
        out_shape=[jax.ShapeDtypeStruct((block, width), jnp.bfloat16)] * count,
        in_specs=[anywhere] * (count + 3 * pieces) + [inside] * 5,
        out_specs=[inside] * count,
        scratch_shapes=[
            pltpu.VMEM((everything, wide), jnp.bfloat16),
            pltpu.VMEM((pieces, units, width), jnp.bfloat16),
            pltpu.VMEM((pieces, units, width), jnp.bfloat16),
            pltpu.VMEM((pieces, units, width), jnp.bfloat16),
            pltpu.VMEM((pieces, everything, units), jnp.bfloat16),
            pltpu.VMEM((everything, shared_units), jnp.bfloat16),
            pltpu.VMEM((everything, side_units), jnp.bfloat16),
            pltpu.SemaphoreType.DMA((4, max(count, pieces))),
        ],
        compiler_params=pltpu.CompilerParams(vmem_limit_bytes=56 * 1024 * 1024),
        cost_estimate=pl.CostEstimate(
            flops=flops, transcendentals=0, bytes_accessed=6 * pieces * units * width
        ),
    )(*rows, *gates, *ups, *downs, shared_up_gate, shared_down, side_in, side_out, select)


def body(
    tokens,
    norm_gain,
    expert_ids,
    route_weights,
    expert_gate,
    expert_up,
    expert_down,
    shared_gate,
    shared_up,
    shared_down,
    side_in,
    side_out,
    side_gate,
):
    groups, members = lax.axis_size("ep"), lax.axis_size("tp")
    rank = lax.axis_index("ep")
    local_experts, hidden_part, width = expert_gate.shape
    experts_all = groups * local_experts
    zs = 1
    while zs * zs < groups:
        zs *= 2
    xs, ys = groups // zs, members // cores

    def over_tp(piece):
        same = [piece] + [rotate(piece, "tp", ys, cores, r, 0) for r in range(1, ys)]
        return [q for p in same for q in (p, rotate(p, "tp", ys, cores, 0, 1))]

    normed = normalize(tokens, norm_gain)
    chosen = expert_ids[:, :, None] == jnp.arange(experts_all, dtype=jnp.int32)[None, None, :]
    dense = jnp.sum(jnp.where(chosen, route_weights[:, :, None], 0.0), axis=1)
    opening = jax.nn.sigmoid(jnp.dot(normed, side_gate, preferred_element_type=jnp.float32))
    factors = jnp.concatenate([dense, opening[:, None]], axis=1)
    factor_count = experts_all + 1
    high = lax.reduce_precision(factors, 8, 7)
    low = factors - high
    tail = -(-2 * factor_count // lanes) * lanes
    packed = jnp.pad(jnp.concatenate([high, low], axis=1), ((0, 0), (0, tail - 2 * factor_count)))
    row = jnp.concatenate([normed, packed.astype(jnp.bfloat16)], axis=1)
    row, side_in, side_out = lax.optimization_barrier((row, side_in, side_out))

    along_z = [row] + [rotate(row, "ep", zs, xs, r, 0) for r in range(1, zs)]
    rows = [[r] + [rotate(r, "ep", zs, xs, 0, d) for d in range(1, xs)] for r in along_z]

    flat = [w.reshape(local_experts * hidden_part, width) for w in (expert_gate, expert_up, expert_down)]
    gates, ups, downs = [over_tp(w) for w in flat]

    unit_count = shared_gate.shape[0] // groups
    shared = jnp.stack(
        [
            lax.dynamic_slice_in_dim(w, rank * unit_count, unit_count, axis=0)
            for w in (shared_gate, shared_up, shared_down)
        ]
    )
    shared = jnp.concatenate(over_tp(shared), axis=1)
    both = shared[:2].reshape(2 * unit_count * members, width)

    side_units = side_in.shape[1] // groups
    core = lax.axis_index("tp") % cores
    half = side_in.shape[0] // cores
    side = jnp.stack(
        [lax.dynamic_slice_in_dim(w, core * half, half, axis=0) for w in (side_in, side_out)]
    ).reshape(2, half, groups, side_units)
    side = lax.all_to_all(side, "ep", split_axis=2, concat_axis=1, tiled=True)
    side = side.reshape(2, groups, half, side_units)
    other = rotate(side, "tp", ys, cores, 0, 1)
    side = jnp.where(
        core == 0, jnp.stack([side, other], axis=2), jnp.stack([other, side], axis=2)
    ).reshape(2, width, side_units)

    units = local_experts * hidden_part
    place = jnp.arange(members * units + side_units, dtype=jnp.int32)
    factor = jnp.where(
        place < members * units, rank * local_experts + place // hidden_part % local_experts, experts_all
    )
    index = jnp.arange(tail, dtype=jnp.int32)[:, None]
    select = ((index == factor) | (index == factor + factor_count)).astype(jnp.bfloat16)

    collected, waiting = {}, []
    for t in range(zs):
        now = rows[t]
        if len(waiting) > 1:
            now, waiting[-2] = lax.optimization_barrier((now, waiting[-2]))
            collected[t - 2] = waiting[-2]
        blocks = experts(now, gates, ups, downs, both, shared[2], side[0], side[1], select)
        total = blocks[0].astype(jnp.float32)
        for d in range(1, xs):
            total += rotate(blocks[d], "ep", zs, xs, 0, -d).astype(jnp.float32)
        waiting.append(total.astype(jnp.bfloat16) if t else total)
        collected[t] = waiting[-1]
    for t in range(1, zs):
        collected[t] = rotate(collected[t], "ep", zs, xs, -t, 0)
    mixed = collected[0]
    for t in range(1, zs):
        mixed += collected[t].astype(jnp.float32)
    return mixed.astype(jnp.bfloat16)


def solution(mesh):
    placed = (
        P(("ep", "tp"), None),
        P(),
        P(("ep", "tp"), None),
        P(("ep", "tp"), None),
        P("ep", "tp", None),
        P("ep", "tp", None),
        P("ep", "tp", None),
        P("tp", None),
        P("tp", None),
        P("tp", None),
        P("ep", None),
        P("ep", None),
        P(),
    )
    return jax.shard_map(
        body, mesh=mesh, in_specs=placed, out_specs=P(("ep", "tp"), None), check_vma=False
    )
```
